256 devices in a mesh: sp: 32 (over z, y), tp: 8 (over x, core).
Axes of the slice: x: 4, y: 4, z: 8, core: 2. Of those that a mesh axis runs over, the one named last changes fastest.
Arguments:
- queries: bfloat16 [9216, 2048], P('sp', 'tp'), as said below
- key_vectors: bfloat16 [9216, 2048], P('sp', 'tp'), as said below
- latents: bfloat16 [9216, 2048], P('sp'), as said below
- value_weight: bfloat16 [2048, 2048], P(None, 'tp'), as said below
- log_sums: float32 [9216, 32], P('sp', 'tp'), as said below
- out_first: bfloat16 [9216, 2048], P('sp', 'tp'), as said below
- out_second: bfloat16 [9216, 2048], P('sp', 'tp'), as said below
- cotangent: bfloat16 [9216, 2048], P('sp', 'tp'), may hold values from -6 to 6
- head_lambda: float32 [16], P('tp'), may hold values from 0.3 to 0.8
Outputs:
- grad_queries: float32 [9216, 2048], P('sp', 'tp')
- grad_keys: float32 [9216, 2048], P('sp', 'tp')
- grad_latents: bfloat16 [9216, 2048], P('sp', 'tp')
- grad_weight: float32 [2048, 2048], P('sp', 'tp')
The draws below stay inside these ranges and needn't reach their ends.
Inputs may be any that keep to these rules, and one draw needn't show every extreme that they name: queries with entries of standard deviation 1.75. `key_vectors`: keys with entries of standard deviation 1. `latents`: inputs of standard deviation 1. `value_weight`: weights scaled by the inverse square root of 2048. `log_sums`: each row's log-sum of exponentials of its causal scores, for the given queries and keys. `out_first`: the first map's attention output for the given queries, keys, values and log-sums. `out_second`: the second map's attention output, likewise.
All inputs are finite; a program needn't handle non-finite values.
Results may differ from the reference program's by a relative error of at most 0.022.
Values may be sent and summed in bfloat16 or wider, within the bound.
A program may use at most 192 MiB of HBM per device.

```python
import jax
import jax.numpy as jnp
from jax import lax

D = 2048
HEADS = 16
DH = 64
DV = 128
TOK_DEV = 288
TOKENS = 9216
N_SP = 32
N_TP = 8


def build_inputs(key):
    queries = (1.75 * jax.random.normal(jax.random.fold_in(key, 101), (TOKENS, HEADS * 2 * DH), jnp.float32)).astype(jnp.bfloat16)
    key_vectors = jax.random.normal(jax.random.fold_in(key, 102), (TOKENS, HEADS * 2 * DH), jnp.float32).astype(jnp.bfloat16)
    latents = jax.random.normal(jax.random.fold_in(key, 103), (TOKENS, D), jnp.float32).astype(jnp.bfloat16)
    value_weight = (jax.random.normal(jax.random.fold_in(key, 104), (D, HEADS * DV), jnp.float32) * D ** (-0.5)).astype(jnp.bfloat16)
    values = jnp.dot(latents, value_weight, preferred_element_type=jnp.float32).astype(jnp.bfloat16)
    blocks = TOKENS // TOK_DEV
    query_heads = queries.astype(jnp.float32).reshape(blocks, TOK_DEV, HEADS, 2, DH)
    key_heads = key_vectors.astype(jnp.float32).reshape(TOKENS, HEADS, 2, DH)
    value_heads = values.astype(jnp.float32).reshape(TOKENS, HEADS, DV)
    positions = jnp.arange(TOKENS, dtype=jnp.int32)

    def one_block(pair):
        block_rows, block_index = pair
        query_pos = block_index * TOK_DEV + jnp.arange(TOK_DEV, dtype=jnp.int32)
        scores = jnp.einsum('nhad,mhad->hanm', block_rows, key_heads) * DH ** (-0.5)
        causal = query_pos[:, None] >= positions[None, :]
        scores = jnp.where(causal, scores, -1e+30)
        highest = jnp.max(scores, axis=-1, keepdims=True)
        expo = jnp.exp(scores - highest)
        total = jnp.sum(expo, axis=-1, keepdims=True)
        outputs = jnp.einsum('hanm,mhe->nhae', expo / total, value_heads)
        sums = (highest + jnp.log(total))[..., 0].transpose(2, 0, 1)
        return (sums, outputs)
    sums, outputs = lax.map(one_block, (query_heads, jnp.arange(blocks, dtype=jnp.int32)))
    log_sums = sums.reshape(TOKENS, HEADS * 2)
    out_first = outputs[:, :, :, 0, :].reshape(TOKENS, HEADS * DV).astype(jnp.bfloat16)
    out_second = outputs[:, :, :, 1, :].reshape(TOKENS, HEADS * DV).astype(jnp.bfloat16)
    return (queries, key_vectors, latents, value_weight, log_sums, out_first, out_second)


def draw_queries(key, part):
    return build_inputs(key)[0]


def draw_key_vectors(key, part):
    return build_inputs(key)[1]


def draw_latents(key, part):
    return build_inputs(key)[2]


def draw_value_weight(key, part):
    return build_inputs(key)[3]


def draw_log_sums(key, part):
    return build_inputs(key)[4]


def draw_out_first(key, part):
    return build_inputs(key)[5]


def draw_out_second(key, part):
    return build_inputs(key)[6]


def strengthened(entries, key, source, target, shards_of, factor):
    def block_of(dim):
        return (jnp.arange(entries.shape[dim]) // (entries.shape[dim] // shards_of)).reshape((-1,) + (1,) * (entries.ndim - 1 - dim))

    one_side = jax.random.permutation(key, shards_of)[block_of(target)]
    far = (block_of(target) + shards_of // 2) % shards_of
    return jnp.where((block_of(source) == one_side) | (block_of(source) == far), factor * entries, entries)


def block_scale(key, extent, shards, least, largest):
    factor_of = 1.0
    for dim, blocks in shards:
        steps = jax.random.uniform(jax.random.fold_in(jax.random.fold_in(key, 6), dim), (blocks,), jnp.float32, least / len(shards), largest / len(shards))
        factor_of = factor_of * jnp.repeat(jnp.exp(steps), extent[dim] // blocks).reshape((-1,) + (1,) * (len(extent) - 1 - dim))
    return factor_of


def noise_with(own_key, extent, spread, limit, cuts, heavy, kind=jnp.bfloat16):
    result = spread * jax.random.normal(own_key, extent, jnp.float32)
    if cuts:
        result = result * block_scale(own_key, extent, cuts, -0.22, 0.18)
    return jnp.clip(strengthened(result, jax.random.fold_in(own_key, 3), *heavy), -limit, limit).astype(kind)


def setup_inputs(seed: int = 0) -> dict:
    arg_keys = jax.random.split(jax.random.key(seed), 10)
    return {
        "queries": draw_queries(jax.random.fold_in(arg_keys[9], 71), 0),
        "key_vectors": draw_key_vectors(jax.random.fold_in(arg_keys[9], 71), 0),
        "latents": draw_latents(jax.random.fold_in(arg_keys[9], 71), 0),
        "value_weight": draw_value_weight(jax.random.fold_in(arg_keys[9], 71), 0),
        "log_sums": draw_log_sums(jax.random.fold_in(arg_keys[9], 71), 0),
        "out_first": draw_out_first(jax.random.fold_in(arg_keys[9], 71), 0),
        "out_second": draw_out_second(jax.random.fold_in(arg_keys[9], 71), 0),
        "cotangent": noise_with(arg_keys[7], (TOKENS, HEADS * DV), 1.0, 6.0, ((0, 32), (1, 8)), (0, 1, 32, 2.75)),
        "head_lambda": jnp.clip(0.3 + 0.5 * jax.random.uniform(arg_keys[8], (HEADS,), jnp.float32) ** block_scale(arg_keys[8], (HEADS,), ((0, 8),), -0.2, 0.2), 0.3, 0.8),
    }


def row_terms(out_first, out_second, cotangent, head_lambda):
    count = out_first.shape[0]
    head_count = head_lambda.shape[0]
    first = out_first.astype(jnp.float32).reshape(count, head_count, DV)
    second = out_second.astype(jnp.float32).reshape(count, head_count, DV)
    mixed = first - head_lambda[None, :, None] * second
    inverse = lax.rsqrt(lax.optimization_barrier(jnp.mean(mixed * mixed, axis=-1, keepdims=True)) + 1e-06)
    normed = mixed * inverse
    grad_out = cotangent.astype(jnp.float32).reshape(count, head_count, DV)
    grad_mixed = inverse * (grad_out - normed * lax.optimization_barrier(jnp.mean(grad_out * normed, axis=-1, keepdims=True)))
    grad_rows = grad_mixed.astype(jnp.bfloat16)
    widened = lax.optimization_barrier(grad_rows).astype(jnp.float32)
    row_dots = jnp.stack([lax.optimization_barrier(jnp.sum(widened * first, axis=-1)), lax.optimization_barrier(jnp.sum(widened * second, axis=-1))], axis=-1)
    return (grad_rows.reshape(count, head_count * DV), row_dots.reshape(count, head_count * 2))

def block_grads(query_rows, grad_rows, lse_rows, dot_rows, query_pos, key_rows, value_rows, key_pos, head_lambda):
    count = query_rows.shape[0]
    width = key_rows.shape[0]
    head_count = head_lambda.shape[0]
    score_scale = DH ** (-0.5)
    query_heads = query_rows.astype(jnp.float32).reshape(count, head_count, 2, DH)
    key_heads = key_rows.astype(jnp.float32).reshape(width, head_count, 2, DH)
    grad_heads = grad_rows.astype(jnp.float32).reshape(count, head_count, DV)
    value_heads = value_rows.astype(jnp.float32).reshape(width, head_count, DV)
    scores = jnp.einsum('nhad,mhad->hanm', query_heads, key_heads) * score_scale
    causal = query_pos[:, None] >= key_pos[None, :]
    shifts = lse_rows.reshape(count, head_count, 2).transpose(1, 2, 0)[..., None]
    probs = jnp.exp(jnp.where(causal, scores - shifts, -1e+30))
    d_attn = jnp.einsum('nhe,mhe->hnm', grad_heads, value_heads)
    dots = dot_rows.reshape(count, head_count, 2).transpose(1, 2, 0)[..., None]
    map_weight = jnp.stack([jnp.ones_like(head_lambda), -head_lambda], axis=1)[:, :, None, None]
    d_scores = (map_weight * probs * (d_attn[:, None] - dots)).astype(jnp.bfloat16)
    d_scores = lax.optimization_barrier(d_scores).astype(jnp.float32)
    weights = (probs[:, 0] - head_lambda[:, None, None] * probs[:, 1]).astype(jnp.bfloat16)
    weights = lax.optimization_barrier(weights).astype(jnp.float32)
    grad_q = jnp.einsum('hanm,mhad->nhad', d_scores, key_heads) * score_scale
    grad_k = jnp.einsum('hanm,nhad->mhad', d_scores, query_heads) * score_scale
    grad_v = jnp.einsum('hnm,nhe->mhe', weights, grad_heads)
    return (grad_q.reshape(count, -1), grad_k.reshape(width, -1), grad_v.reshape(width, -1))

def reference(queries, key_vectors, latents, value_weight, log_sums, out_first, out_second, cotangent, head_lambda):
    values = jnp.dot(latents, value_weight, preferred_element_type=jnp.float32).astype(jnp.bfloat16)
    grad_rows, row_dots = row_terms(out_first, out_second, cotangent, head_lambda)
    positions = jnp.arange(TOKENS, dtype=jnp.int32)

    def per_head(index):
        query_head = lax.dynamic_slice_in_dim(queries, index * 2 * DH, 2 * DH, 1)
        key_head = lax.dynamic_slice_in_dim(key_vectors, index * 2 * DH, 2 * DH, 1)
        value_head = lax.dynamic_slice_in_dim(values, index * DV, DV, 1)
        grad_head = lax.dynamic_slice_in_dim(grad_rows, index * DV, DV, 1)
        lse_head = lax.dynamic_slice_in_dim(log_sums, index * 2, 2, 1)
        dot_head = lax.dynamic_slice_in_dim(row_dots, index * 2, 2, 1)
        lambda_one = lax.dynamic_slice_in_dim(head_lambda, index, 1, 0)

        def block_step(totals, block_index):
            first_row = (block_index * TOK_DEV).astype(jnp.int32)
            query_pos = first_row + jnp.arange(TOK_DEV, dtype=jnp.int32)
            grad_q, grad_k, grad_v = block_grads(lax.dynamic_slice_in_dim(query_head, first_row, TOK_DEV, 0), lax.dynamic_slice_in_dim(grad_head, first_row, TOK_DEV, 0), lax.dynamic_slice_in_dim(lse_head, first_row, TOK_DEV, 0), lax.dynamic_slice_in_dim(dot_head, first_row, TOK_DEV, 0), query_pos, key_head, value_head, positions, lambda_one)
            return ((totals[0] + grad_k, totals[1] + grad_v), grad_q)
        initial = (jnp.zeros((TOKENS, 2 * DH), jnp.float32), jnp.zeros((TOKENS, DV), jnp.float32))
        totals, grad_blocks = lax.scan(block_step, initial, jnp.arange(N_SP, dtype=jnp.int32))
        return (grad_blocks.reshape(TOKENS, 2 * DH), totals[0], totals[1])
    grad_q, grad_k, grad_v = lax.map(per_head, jnp.arange(HEADS, dtype=jnp.int32))
    grad_queries = grad_q.transpose(1, 0, 2).reshape(TOKENS, HEADS * 2 * DH)
    grad_keys = grad_k.transpose(1, 0, 2).reshape(TOKENS, HEADS * 2 * DH)
    grad_values = grad_v.transpose(1, 0, 2).reshape(TOKENS, HEADS * DV).astype(jnp.bfloat16)
    grad_weight = lax.dot_general(latents, grad_values, (((0,), (0,)), ((), ())), preferred_element_type=jnp.float32)
    value_groups = grad_values.reshape(TOKENS, N_TP, -1).transpose(1, 0, 2)
    weight_groups = value_weight.reshape(D, N_TP, -1).transpose(1, 0, 2)

    def add_group(total, pair):
        partial_sum = lax.dot_general(pair[0], pair[1], (((1,), (1,)), ((), ())), preferred_element_type=jnp.float32)
        rounded = lax.optimization_barrier(partial_sum.astype(jnp.bfloat16))
        return (total + rounded.astype(jnp.float32), None)
    latent_total, unused = lax.scan(add_group, jnp.zeros((TOKENS, D), jnp.float32), (value_groups, weight_groups))
    return (grad_queries, grad_keys, latent_total.astype(jnp.bfloat16), grad_weight)
```

```python
import functools
import math

import jax
import jax.numpy as jnp
from jax import lax
from jax.experimental import pallas as pl
from jax.experimental.pallas import tpu as pltpu
from jax.sharding import PartitionSpec as P

DH = 64
DV = 128
NY = 4
NZ = 8
LOG2E = math.log2(math.e)
BF = jnp.bfloat16
F32 = jnp.float32


def cut_along(x, dim, devices):
    before, after = (x.shape[:dim], x.shape[dim + 1 :])
    return jnp.moveaxis(x.reshape(*before, devices, -1, *after), dim, 0)


def summed_on_arrival(x, axis, dim):
    parts = cut_along(x, dim, lax.axis_size(axis))
    arrived = lax.all_to_all(parts, axis, split_axis=0, concat_axis=0, tiled=True)
    return arrived.astype(jnp.float32).sum(axis=0)


def row_terms(out_first, out_second, cotangent, head_lambda):
    count = out_first.shape[0]
    head_count = head_lambda.shape[0]
    first = out_first.astype(jnp.float32).reshape(count, head_count, DV)
    second = out_second.astype(jnp.float32).reshape(count, head_count, DV)
    mixed = first - head_lambda[None, :, None] * second
    inverse = lax.rsqrt(jnp.mean(mixed * mixed, axis=-1, keepdims=True) + 1e-06)
    normed = mixed * inverse
    grad_out = cotangent.astype(jnp.float32).reshape(count, head_count, DV)
    grad_mixed = inverse * (grad_out - normed * jnp.mean(grad_out * normed, axis=-1, keepdims=True))
    grad_rows = grad_mixed.astype(jnp.bfloat16)
    widened = lax.optimization_barrier(grad_rows).astype(jnp.float32)
    row_dots = jnp.stack(
        [jnp.sum(widened * first, axis=-1), jnp.sum(widened * second, axis=-1)], axis=-1
    )
    return (grad_rows.reshape(count, head_count * DV), row_dots.reshape(count, head_count * 2))


def dot(a, b):
    return jnp.dot(a, b, preferred_element_type=F32)


def low_map(x):
    return lax.broadcasted_iota(jnp.int32, x.shape, 1) < DH


def score_terms(m_a, m_b, na_t, nb_t, shift0, shift1, dot0, dot1, mask):
    low = low_map(m_a)
    none = jnp.zeros_like(m_a)
    s0 = dot(jnp.where(low, m_a, none), na_t) * (LOG2E * DH ** (-0.5)) - shift0
    s1 = dot(jnp.where(low, none, m_a), na_t) * (LOG2E * DH ** (-0.5)) - shift1
    da = dot(m_b, nb_t)
    if mask is not None:
        s0 = jnp.where(mask, s0, -1e30)
        s1 = jnp.where(mask, s1, -1e30)
    p0 = jnp.exp2(s0)
    p1 = jnp.exp2(s1)
    ds0 = (p0 * (da - dot0)).astype(BF)
    ds1 = (p1 * (dot1 - da)).astype(BF)
    weights = (p0 - p1).astype(BF)
    return ds0, ds1, weights


def attention_kernel(
    ma_ref, na_ref, mb_ref, nb_ref, sta_ref, stb_ref,
    gq_ref, gk_ref, gv_ref,
    ma, mb, sta, stb, na, nb, nat, nvt, nbt, ndt,
    acc_a, acc_v, acc_b, own_a, own_b,
    full_a, full_b, send_a, send_b, recv_a, recv_b, nsend_a, nsend_b, nrecv_a, nrecv_b,
    yg_send, yg_recv, ma_send, ma_recv, sta_send, sta_recv, mb_send, mb_recv,
    ra_send, ra_recv, rb_send, rb_recv, na_send, na_recv, nb_send, nb_recv,
):
    rows = ma_ref.shape[0]
    wide = NY * rows
    sp = lax.axis_index("sp")
    z = sp // NY
    y = sp % NY

    def copy(src, dst, ssem, rsem, target):
        return pltpu.make_async_remote_copy(
            src_ref=src, dst_ref=dst, send_sem=ssem, recv_sem=rsem,
            device_id={"sp": target}, device_id_type=pl.DeviceIdType.MESH,
        )

    barrier = pltpu.get_barrier_semaphore()
    y_peers = [z * NY + (y + k) % NY for k in range(1, NY)]
    z_peers = [((z + k) % NZ) * NY + y for k in range(1, NZ)]
    for peer in y_peers + z_peers:
        pl.semaphore_signal(barrier, inc=1, device_id={"sp": peer}, device_id_type=pl.DeviceIdType.MESH)
    pl.semaphore_wait(barrier, len(y_peers) + len(z_peers))

    def span(index):
        return pl.ds(pl.multiple_of(index * rows, rows), rows)

    below = jnp.maximum(sp - NY, 0)
    above = jnp.minimum(sp + NY, NZ * NY - 1)

    def ma_copy(src, c):
        return copy(src, ma.at[c], ma_send.at[c], ma_recv.at[c], below)

    def sta_copy(src, c):
        return copy(src, sta.at[c], sta_send.at[c], sta_recv.at[c], below)

    def mb_copy(src, c):
        return copy(src, mb.at[c], mb_send.at[c], mb_recv.at[c], above)

    def y_copies(k, slot, target):
        return [
            copy(na_ref, na.at[span(slot)], yg_send.at[k, 0], yg_recv.at[slot, 0], target),
            copy(nb_ref, nb.at[span(slot)], yg_send.at[k, 1], yg_recv.at[slot, 1], target),
            copy(stb_ref, stb.at[slot], yg_send.at[k, 2], yg_recv.at[slot, 2], target),
        ]

    for k, peer in enumerate(y_peers):
        for c in y_copies(k, y, peer):
            c.start()

    @pl.when(z > 0)
    def _():
        sta_copy(sta_ref, z).start()
        ma_copy(ma_ref, z).start()

    @pl.when(z < NZ - 1)
    def _():
        mb_copy(mb_ref, z).start()

    na[span(y), :] = na_ref[...]
    nb[span(y), :] = nb_ref[...]
    stb[y] = stb_ref[...]

    for k, peer in enumerate(y_peers):
        for c in y_copies(k, (y + k + 1) % NY, peer):
            c.wait_recv()

    nat[...] = na[:, :DV].T
    nvt[...] = na[:, DV:].T
    nbt[...] = nb[:, :DV].T
    ndt[...] = nb[:, DV:].T
    stb[NY] = stb[0] + stb[1] + stb[2] + stb[3]

    def take_a(t):
        sta_copy(sta.at[z + t], z + t).wait_recv()
        ma_copy(ma.at[z + t], z + t).wait_recv()

    def take_b(t):
        mb_copy(mb.at[z - t], z - t).wait_recv()

    def pass_a(t):
        @pl.when(jnp.logical_and(z > 0, z + t < NZ))
        def _():
            take_a(t)
            sta_copy(sta.at[z + t], z + t).start()
            ma_copy(ma.at[z + t], z + t).start()

    def pass_b(t):
        @pl.when(jnp.logical_and(z < NZ - 1, z - t >= 0))
        def _():
            take_b(t)
            mb_copy(mb.at[z - t], z - t).start()

    def unit_a(m, stats, mask):
        st = stats.T[:rows]
        m_a = m[:, :DV]
        m_b = m[:, DV:]
        ds0, ds1, weights = score_terms(
            m_a, m_b, nat[...], nvt[...], st[:, 0:1], st[:, 1:2], st[:, 2:3], st[:, 3:4], mask
        )
        k_all = na[:, :DV]
        d0 = dot(ds0, k_all)
        d1 = dot(ds1, k_all)
        m_at = m_a.T
        parts = (dot(m_at[:DH], ds0), dot(m_at[DH:], ds1), dot(m_b.T, weights))
        return jnp.where(low_map(d0), d0, d1), parts

    def unit_b(m, mask):
        st = stb[NY]
        m_a = m[:, :DV]
        m_b = m[:, DV:]
        ds0, ds1, weights = score_terms(
            m_a, m_b, nbt[...], ndt[...], st[0:1], st[1:2], st[2:3], st[3:4], mask
        )
        q_all = nb[:, :DV]
        d0 = dot(ds0, q_all)
        d1 = dot(ds1, q_all)
        dv = dot(weights, nb[:, DV:])
        m_at = m_a.T
        parts = (dot(m_at[:DH], ds0), dot(m_at[DH:], ds1))
        return jnp.where(low_map(d0), d0, d1), dv, parts

    lane = lax.broadcasted_iota(jnp.int32, (rows, wide), 1)
    place = lax.broadcasted_iota(jnp.int32, (rows, wide), 0) + y * rows

    pass_a(1)
    pass_b(1)
    moved, parts = unit_a(ma_ref[...], sta_ref[...], place >= lane)
    own_a[...] = moved
    acc_a[:DH] = parts[0]
    acc_a[DH:] = parts[1]
    acc_v[...] = parts[2]
    moved, moved_v, parts = unit_b(mb_ref[...], lane >= place)
    own_b[:, :DV] = moved
    own_b[:, DV:] = moved_v
    acc_b[:DH] = parts[0]
    acc_b[DH:] = parts[1]

    def out_a(t):
        return copy(
            send_a.at[t], recv_a.at[z], ra_send.at[t], ra_recv.at[z], jnp.minimum(sp + t * NY, NZ * NY - 1)
        )

    def out_b(t):
        return copy(
            send_b.at[t], recv_b.at[z], rb_send.at[t], rb_recv.at[z], jnp.maximum(sp - t * NY, 0)
        )

    def step(t, carry):
        pass_a(t + 1)
        pass_b(t + 1)

        @pl.when(z + t < NZ)
        def _():
            @pl.when(z == 0)
            def _():
                take_a(t)

            moved, parts = unit_a(ma[z + t], sta[z + t], None)
            send_a[t] = moved.astype(BF)
            out_a(t).start()
            acc_a[:DH] += parts[0]
            acc_a[DH:] += parts[1]
            acc_v[...] += parts[2]

        @pl.when(z - t >= 0)
        def _():
            @pl.when(z == NZ - 1)
            def _():
                take_b(t)

            moved, moved_v, parts = unit_b(mb[z - t], None)
            send_b[t, :, :DV] = moved.astype(BF)
            send_b[t, :, DV:] = moved_v.astype(BF)
            out_b(t).start()
            acc_b[:DH] += parts[0]
            acc_b[DH:] += parts[1]

        return carry

    lax.fori_loop(1, NZ, step, 0)

    def y_out_a(k, mine, theirs, target):
        return copy(nsend_a.at[span(theirs)], nrecv_a.at[mine], na_send.at[k], na_recv.at[mine], target)

    def y_out_b(k, mine, theirs, target):
        return copy(nsend_b.at[span(theirs)], nrecv_b.at[mine], nb_send.at[k], nb_recv.at[mine], target)

    full_a[:, :DV] = acc_a[...].T
    full_a[:, DV:] = acc_v[...].T
    nsend_a[...] = full_a[...].astype(BF)
    for k, peer in enumerate(y_peers):
        y_out_a(k, y, (y + k + 1) % NY, peer).start()
    full_b[...] = acc_b[...].T
    nsend_b[...] = full_b[...].astype(BF)
    for k, peer in enumerate(y_peers):
        y_out_b(k, y, (y + k + 1) % NY, peer).start()

    def add_a(j, carry):
        copy(send_a.at[0], recv_a.at[j], ra_send.at[0], ra_recv.at[j], below).wait_recv()
        own_a[...] += recv_a[j].astype(F32)
        return carry

    def add_b(j, carry):
        copy(send_b.at[0], recv_b.at[j], rb_send.at[0], rb_recv.at[j], above).wait_recv()
        own_b[...] += recv_b[j].astype(F32)
        return carry

    lax.fori_loop(0, z, add_a, 0)
    lax.fori_loop(z + 1, NZ, add_b, 0)

    total_a = full_a[span(y), :]
    total_b = full_b[span(y), :]
    for k, peer in enumerate(y_peers):
        slot = (y + k + 1) % NY
        y_out_a(k, slot, y, peer).wait_recv()
        total_a += nrecv_a[slot].astype(F32)
    gv_ref[:, :DV] = total_a[:, DV:].astype(BF)
    gv_ref[:, DV:] = own_b[:, DV:].astype(BF)
    scale = DH ** (-0.5)
    gk_ref[:, :DV] = total_a[:, :DV] * scale
    gk_ref[:, DV:] = own_b[:, :DV] * scale
    for k, peer in enumerate(y_peers):
        slot = (y + k + 1) % NY
        y_out_b(k, slot, y, peer).wait_recv()
        total_b += nrecv_b[slot].astype(F32)
    gq_ref[:, :DV] = own_a[...] * scale
    gq_ref[:, DV:] = total_b * scale

    for k, peer in enumerate(y_peers):
        for c in y_copies(k, y, peer):
            c.wait_send()
        y_out_a(k, y, y, peer).wait_send()
        y_out_b(k, y, y, peer).wait_send()

    def drain_a(t, carry):
        @pl.when(t > 0)
        def _():
            out_a(t).wait_send()

        @pl.when(z > 0)
        def _():
            sta_copy(sta.at[z + t], z + t).wait_send()
            ma_copy(ma.at[z + t], z + t).wait_send()

        return carry

    def drain_b(t, carry):
        @pl.when(t > 0)
        def _():
            out_b(t).wait_send()

        @pl.when(z < NZ - 1)
        def _():
            mb_copy(mb.at[z - t], z - t).wait_send()

        return carry

    lax.fori_loop(0, NZ - z, drain_a, 0)
    lax.fori_loop(0, z + 1, drain_b, 0)


def attention(ma, na, mb, nb, sta, stb):
    rows = ma.shape[0]
    wide = NY * rows
    dma = pltpu.SemaphoreType.DMA
    vmem = pltpu.VMEM
    whole = pl.BlockSpec(memory_space=pltpu.VMEM)
    return pl.pallas_call(
        attention_kernel,
        out_shape=(
            jax.ShapeDtypeStruct((rows, 2 * DV), F32),
            jax.ShapeDtypeStruct((rows, 2 * DV), F32),
            jax.ShapeDtypeStruct((rows, 2 * DV), BF),
        ),
        in_specs=[whole] * 6,
        out_specs=(whole,) * 3,
        scratch_shapes=[
            vmem((NZ, rows, 2 * DV), BF),
            vmem((NZ, rows, 2 * DV), BF),
            vmem((NZ,) + sta.shape, F32),
            vmem((NY + 1,) + stb.shape, F32),
            vmem((wide, 2 * DV), BF),
            vmem((wide, 2 * DV), BF),
            vmem((DV, wide), BF),
            vmem((DV, wide), BF),
            vmem((DV, wide), BF),
            vmem((DV, wide), BF),
            vmem((DV, wide), F32),
            vmem((DV, wide), F32),
            vmem((DV, wide), F32),
            vmem((rows, DV), F32),
            vmem((rows, 2 * DV), F32),
            vmem((wide, 2 * DV), F32),
            vmem((wide, DV), F32),
            vmem((NZ, rows, DV), BF),
            vmem((NZ, rows, 2 * DV), BF),
            vmem((NZ, rows, DV), BF),
            vmem((NZ, rows, 2 * DV), BF),
            vmem((wide, 2 * DV), BF),
            vmem((wide, DV), BF),
            vmem((NY, rows, 2 * DV), BF),
            vmem((NY, rows, DV), BF),
            dma((NY - 1, 3)),
            dma((NY, 3)),
        ]
        + [dma((NZ,))] * 10
        + [dma((NY,))] * 4,
        compiler_params=pltpu.CompilerParams(
            collective_id=0, has_side_effects=True, vmem_limit_bytes=60 * 1024 * 1024
        ),
        cost_estimate=pl.CostEstimate(flops=20_000_000_000, bytes_accessed=4_000_000, transcendentals=6_000_000),
    )(ma, na, mb, nb, sta, stb)


def per_device(
    queries,
    key_vectors,
    latents,
    value_weight,
    log_sums,
    out_first,
    out_second,
    cotangent,
    head_lambda,
):
    rows = queries.shape[0]
    values = jnp.dot(latents, value_weight, preferred_element_type=jnp.float32).astype(jnp.bfloat16)
    grad_rows, row_dots = row_terms(out_first, out_second, cotangent, head_lambda)
    shifts = log_sums.reshape(rows, 2, 2) * LOG2E
    shifts = shifts - jnp.stack([jnp.zeros_like(head_lambda), jnp.log2(head_lambda)], axis=1)[None]
    stats = jnp.concatenate([shifts, row_dots.reshape(rows, 2, 2)], axis=2)
    stats = jnp.pad(stats.transpose(1, 2, 0), ((0, 0), (0, 4), (0, 0)))
    sta = jnp.pad(stats[0], ((0, 0), (0, -rows % 128)))
    y = lax.axis_index("sp") % NY
    stb = lax.dynamic_update_slice(
        jnp.zeros((8, NY * rows), F32), stats[1], (jnp.int32(0), (y * rows).astype(jnp.int32))
    )
    ma = jnp.concatenate([queries[:, :DV], grad_rows[:, :DV]], axis=1)
    nb = jnp.concatenate([queries[:, DV:], grad_rows[:, DV:]], axis=1)
    na = jnp.concatenate([key_vectors[:, :DV], values[:, :DV]], axis=1)
    mb = jnp.concatenate([key_vectors[:, DV:], values[:, DV:]], axis=1)
    grad_queries, grad_keys, values_grad = attention(ma, na, mb, nb, sta, stb)
    grad_weight = summed_on_arrival(
        lax.dot_general(
            latents, values_grad, (((0,), (0,)), ((), ())), preferred_element_type=jnp.float32
        ).astype(jnp.bfloat16),
        "sp",
        0,
    )
    latent_partial = lax.dot_general(
        values_grad, value_weight, (((1,), (1,)), ((), ())), preferred_element_type=jnp.float32
    )
    grad_latents = lax.psum_scatter(
        latent_partial.astype(jnp.bfloat16), "tp", scatter_dimension=1, tiled=True
    )
    return (grad_queries, grad_keys, grad_latents, grad_weight)


def solution(mesh):
    return jax.shard_map(
        per_device,
        mesh=mesh,
        in_specs=(
            P("sp", "tp"),
            P("sp", "tp"),
            P("sp", None),
            P(None, "tp"),
            P("sp", "tp"),
            P("sp", "tp"),
            P("sp", "tp"),
            P("sp", "tp"),
            P("tp"),
        ),
        out_specs=(P("sp", "tp"), P("sp", "tp"), P("sp", "tp"), P("sp", "tp")),
        check_vma=False,
    )
```

```python
import functools
import math

import jax
import jax.numpy as jnp
from jax import lax
from jax.experimental import pallas as pl
from jax.experimental.pallas import tpu as pltpu
from jax.sharding import PartitionSpec as P

DH = 64
DV = 128
NY = 4
NZ = 8
NX = 4
PIECES = 1
CHAIN = 4
LOG2E = math.log2(math.e)
BF = jnp.bfloat16
F32 = jnp.float32


def dot(a, b):
    return jnp.dot(a, b, preferred_element_type=F32)


def low_map(x):
    return lax.broadcasted_iota(jnp.int32, x.shape, 1) < DH


def score_terms(m_a, m_b, na_t, nb_t, shift0, shift1, dot0, dot1, mask):
    low = low_map(m_a)
    none = jnp.zeros_like(m_a)
    s0 = dot(jnp.where(low, m_a, none), na_t) * (LOG2E * DH ** (-0.5)) - shift0
    s1 = dot(jnp.where(low, none, m_a), na_t) * (LOG2E * DH ** (-0.5)) - shift1
    da = dot(m_b, nb_t)
    if mask is not None:
        s0 = jnp.where(mask, s0, -1e30)
        s1 = jnp.where(mask, s1, -1e30)
    p0 = jnp.exp2(s0)
    p1 = jnp.exp2(s1)
    ds0 = (p0 * (da - dot0)).astype(BF)
    ds1 = (p1 * (dot1 - da)).astype(BF)
    weights = (p0 - p1).astype(BF)
    return ds0, ds1, weights


def attention_kernel(
    q_ref, k_ref, lat_ref, wv_ref, lse_ref, first_ref, second_ref, cot_ref, lam_ref,
    gq_ref, gk_ref, gl_ref, gw_ref,
    ma, mb, sta, stb, stc, stw, na, nb, nat, nvt, nbt, ndt,
    acc_a, acc_v, acc_b, own_a, own_b, full_a, full_b,
    send_a, send_b, home_a, home_b, nsend_a, nsend_b, nrecv_a, nrecv_b,
    lperm, latg, gvg, dw_send, dw_recv, dl_send, dl_core, dl_pair, dl_recv,
    yg_send, yg_recv, ma_send, ma_recv, sta_send, sta_recv, mb_send, mb_recv,
    ra_send, rb_send, ha_recv, hb_recv,
    na_send, na_recv, nb_send, nb_recv,
    lat_send, lat_recv, gv_send, gv_recv, dw_ssem, dw_rsem, dc_send, dc_recv, dx_send, dx_recv,
):
    rows = q_ref.shape[0]
    wide = NY * rows
    sp = lax.axis_index("sp")
    tp = lax.axis_index("tp")
    z = sp // NY
    y = sp % NY
    x = tp // 2
    core = tp % 2

    def copy_to(src, dst, ssem, rsem, where):
        return pltpu.make_async_remote_copy(
            src_ref=src, dst_ref=dst, send_sem=ssem, recv_sem=rsem,
            device_id=where, device_id_type=pl.DeviceIdType.MESH,
        )

    def copy(src, dst, ssem, rsem, target):
        return copy_to(src, dst, ssem, rsem, {"sp": target})

    barrier = pltpu.get_barrier_semaphore()
    y_slots = [(y + k) % NY for k in range(1, NY)]
    z_slots = [(z + k) % NZ for k in range(1, NZ)]
    x_slots = [(x + k) % NX for k in range(1, NX)]
    y_peers = [z * NY + s for s in y_slots]
    z_peers = [s * NY + y for s in z_slots]
    other_core = {"tp": x * 2 + 1 - core}
    x_peers = [{"tp": s * 2 + core} for s in x_slots]
    everyone = [{"sp": p} for p in y_peers + z_peers] + [other_core] + x_peers
    for peer in everyone:
        pl.semaphore_signal(barrier, inc=1, device_id=peer, device_id_type=pl.DeviceIdType.MESH)

    def span(index):
        return pl.ds(pl.multiple_of(index * rows, rows), rows)

    last = NZ * NY - 1
    below = jnp.maximum(sp - NY, 0)
    above = jnp.minimum(sp + NY, last)
    lowest = y
    highest = (NZ - 1) * NY + y

    piece = rows // PIECES

    def ma_copies(src, st, c, target, far=0):
        return [copy(st, sta.at[c], sta_send.at[c, far], sta_recv.at[c], target)] + [
            copy(
                src.at[p * piece : (p + 1) * piece],
                ma.at[c, p * piece : (p + 1) * piece],
                ma_send.at[c, far * PIECES + p],
                ma_recv.at[c, p],
                target,
            )
            for p in range(PIECES)
        ]

    def mb_copies(src, c, target, far=0):
        return [
            copy(
                src.at[p * piece : (p + 1) * piece],
                mb.at[c, p * piece : (p + 1) * piece],
                mb_send.at[c, far * PIECES + p],
                mb_recv.at[c, p],
                target,
            )
            for p in range(PIECES)
        ]

    def y_copies(k, slot, target):
        return [
            lambda: copy(na.at[span(y)], na.at[span(slot)], yg_send.at[k, 0], yg_recv.at[slot, 0], target),
            lambda: copy(nb.at[span(y)], nb.at[span(slot)], yg_send.at[k, 1], yg_recv.at[slot, 1], target),
            lambda: copy(stb.at[y], stb.at[slot], yg_send.at[k, 2], yg_recv.at[slot, 2], target),
        ]

    def start(copies):
        for c in copies:
            c.start()

    values = dot(lat_ref[...], wv_ref[...]).astype(BF)
    k_own = k_ref[...]
    q_own = q_ref[...]
    which = lax.broadcasted_iota(jnp.int32, (rows, DV), 1)

    def row_terms(h):
        cols = slice(h * DV, (h + 1) * DV)
        first = first_ref[:, cols].astype(F32)
        second = second_ref[:, cols].astype(F32)
        grad_out = cot_ref[:, cols].astype(F32)
        lam = jnp.full((rows, 1), lam_ref[h], F32)
        mixed = first - lam * second
        inverse = lax.rsqrt(jnp.mean(mixed * mixed, axis=-1, keepdims=True) + 1e-06)
        normed = mixed * inverse
        mean = jnp.mean(grad_out * normed, axis=-1, keepdims=True)
        grad_rows = (inverse * (grad_out - normed * mean)).astype(BF)
        widened = grad_rows.astype(F32)
        dot0 = jnp.sum(widened * first, axis=-1, keepdims=True)
        dot1 = jnp.sum(widened * second, axis=-1, keepdims=True)
        stats = jnp.where(which < 3, dot0, dot1)
        stats = jnp.concatenate([stats, jnp.zeros((sta.shape[2] - rows, DV), F32)], axis=0)
        return grad_rows, stats.T[: sta.shape[1]]

    def shifts(h, m):
        shift = lse_ref[2 * h + m : 2 * h + m + 1, :] * LOG2E
        if m == 1:
            shift -= jnp.log(jnp.full((1, rows), lam_ref[h], F32)) * LOG2E
        return shift

    na[span(y), :DV] = k_own[:, :DV]
    na[span(y), DV:] = values[:, :DV]
    mb[z, :, :DV] = k_own[:, DV:]
    mb[z, :, DV:] = values[:, DV:]
    grad_rows, stats = row_terms(0)
    ma[z, :, :DV] = q_own[:, :DV]
    ma[z, :, DV:] = grad_rows
    sta[z] = stats
    sta[z, 0:1, :rows] = shifts(0, 0)
    sta[z, 1:2, :rows] = shifts(0, 1)
    grad_rows, stats = row_terms(1)
    nb[span(y), :DV] = q_own[:, DV:]
    nb[span(y), DV:] = grad_rows
    stb[y] = stats
    stb[y, 0:1, :rows] = shifts(1, 0)
    stb[y, 1:2, :rows] = shifts(1, 1)
    block = lat_ref.shape[1] // (NY * NZ)
    quarter = NZ * block
    for j in range(NY):
        for i in range(0, NZ, 2):
            one = (i * NY + j) * block
            two = (i * NY + NY + j) * block
            lperm[:, j * quarter + i * block : j * quarter + (i + 2) * block] = jnp.concatenate(
                [lat_ref[:, one : one + block], lat_ref[:, two : two + block]], axis=1
            )

    pl.semaphore_wait(barrier, len(everyone))

    @pl.when(z > 0)
    def _():
        start(ma_copies(ma.at[z], sta.at[z], z, below))

    @pl.when(z < NZ - 1)
    def _():
        start(mb_copies(mb.at[z], z, above))

    @pl.when(z > CHAIN)
    def _():
        start(ma_copies(ma.at[z], sta.at[z], z, lowest, 1))

    @pl.when(z < NZ - 1 - CHAIN)
    def _():
        start(mb_copies(mb.at[z], z, highest, 1))

    y_gather = [y_copies(k, y, peer) for k, peer in enumerate(y_peers)]
    for part in range(3):
        for k in range(NY - 1):
            y_gather[k][part]().start()

    def columns(index):
        return pl.ds(pl.multiple_of(index * quarter, quarter), quarter)

    def y_arrived(part):
        for k, peer in enumerate(y_peers):
            y_copies(k, y_slots[k], peer)[part]().wait_recv()

    def take_a(t):
        for c in ma_copies(ma.at[z + t], sta.at[z + t], z + t, below):
            c.wait_recv()

    def take_b(t):
        for c in mb_copies(mb.at[z - t], z - t, above):
            c.wait_recv()

    def pass_a(t):
        @pl.when(jnp.logical_and(jnp.logical_and(z > 0, t < CHAIN), z + t < NZ))
        def _():
            for c in ma_copies(ma.at[z + t], sta.at[z + t], z + t, below):
                c.wait_recv()
                c.start()

    def pass_b(t):
        @pl.when(jnp.logical_and(jnp.logical_and(z < NZ - 1, t < CHAIN), z - t >= 0))
        def _():
            for c in mb_copies(mb.at[z - t], z - t, above):
                c.wait_recv()
                c.start()

    def unit_a(m, stats, mask):
        st = stats.T[:rows]
        m_a = m[:, :DV]
        m_b = m[:, DV:]
        ds0, ds1, weights = score_terms(
            m_a, m_b, nat[...], nvt[...], st[:, 0:1], st[:, 1:2], st[:, 2:3], st[:, 3:4], mask
        )
        k_all = na[:, :DV]
        d0 = dot(ds0, k_all)
        d1 = dot(ds1, k_all)
        m_at = m_a.T
        parts = (dot(m_at[:DH], ds0), dot(m_at[DH:], ds1), dot(m_b.T, weights))
        return jnp.where(low_map(d0), d0, d1), parts

    def unit_b(m, mask):
        st = stw[...]
        m_a = m[:, :DV]
        m_b = m[:, DV:]
        ds0, ds1, weights = score_terms(
            m_a, m_b, nbt[...], ndt[...], st[0:1], st[1:2], st[2:3], st[3:4], mask
        )
        q_all = nb[:, :DV]
        d0 = dot(ds0, q_all)
        d1 = dot(ds1, q_all)
        dv = dot(weights, nb[:, DV:])
        m_at = m_a.T
        parts = (dot(m_at[:DH], ds0), dot(m_at[DH:], ds1))
        return jnp.where(low_map(d0), d0, d1), dv, parts

    lane = lax.broadcasted_iota(jnp.int32, (rows, wide), 1)
    place = lax.broadcasted_iota(jnp.int32, (rows, wide), 0) + y * rows

    def lat_copy(k, mine, theirs, target):
        return copy(lperm.at[:, columns(theirs)], latg.at[mine], lat_send.at[k], lat_recv.at[mine], target)

    latg[y] = lperm[:, columns(y)]
    acc_a[...] = jnp.zeros_like(acc_a)
    acc_v[...] = jnp.zeros_like(acc_v)
    acc_b[...] = jnp.zeros_like(acc_b)
    pass_a(1)
    pass_b(1)
    y_arrived(0)
    nat[...] = na[:, :DV].T
    nvt[...] = na[:, DV:].T

    def home_a_copy(t):
        return copy(
            send_a.at[t], home_a.at[t], ra_send.at[t], ha_recv.at[t], jnp.minimum(sp + t * NY, last)
        )

    def home_b_copy(t):
        return copy(
            send_b.at[t], home_b.at[t], rb_send.at[t], hb_recv.at[t], jnp.maximum(sp - t * NY, 0)
        )

    def chains_a(t):
        return jnp.logical_and(t < CHAIN, z > 0)

    def chains_b(t):
        return jnp.logical_and(t < CHAIN, z < NZ - 1)

    def step(n, carry):
        odd = n % 2
        t = odd * ((n + 1) // 2) + (1 - odd) * (NZ - n // 2)
        t = jnp.where(n < 2, 1 - n, t)
        all_seen = jnp.where(t == 0, 0, NY * rows)

        @pl.when(z + t < NZ)
        def _():
            @pl.when(jnp.logical_and(jnp.logical_not(chains_a(t)), t > 0))
            def _():
                take_a(t)

            @pl.when(t > CHAIN + 1)
            def _():
                start(ma_copies(ma.at[z + t], sta.at[z + t], z + t, above))

            moved, parts = unit_a(ma[z + t], sta[z + t], place + all_seen >= lane)
            acc_a[:DH] += parts[0]
            acc_a[DH:] += parts[1]
            acc_v[...] += parts[2]

            @pl.when(t > 0)
            def _():
                send_a[t] = moved.astype(BF)
                home_a_copy(t).start()

            @pl.when(t == 0)
            def _():
                own_a[...] = moved

        @pl.when(n < 2)
        def _():
            pass_a(n + 2)
            pass_b(n + 2)

        @pl.when(n == 0)
        def _():
            y_arrived(1)
            y_arrived(2)
            nbt[...] = nb[:, :DV].T
            ndt[...] = nb[:, DV:].T
            for j in range(NY):
                stc[j * rows : (j + 1) * rows, : stb.shape[1]] = stb[j].T[:rows]
            stw[...] = stc[...].T[: stw.shape[0]]
            for k, peer in enumerate(y_peers):
                lat_copy(k, y, y_slots[k], peer).start()

        @pl.when(z - t >= 0)
        def _():
            @pl.when(jnp.logical_and(jnp.logical_not(chains_b(t)), t > 0))
            def _():
                take_b(t)

            @pl.when(t > CHAIN + 1)
            def _():
                start(mb_copies(mb.at[z - t], z - t, below))

            moved, moved_v, parts = unit_b(mb[z - t], lane + all_seen >= place)
            acc_b[:DH] += parts[0]
            acc_b[DH:] += parts[1]

            @pl.when(t > 0)
            def _():
                send_b[t, :, :DV] = moved.astype(BF)
                send_b[t, :, DV:] = moved_v.astype(BF)
                home_b_copy(t).start()

            @pl.when(t == 0)
            def _():
                own_b[:, :DV] = moved
                own_b[:, DV:] = moved_v

        return carry

    lax.fori_loop(0, NZ, step, 0)

    def y_out_a(k, mine, theirs, target):
        return copy(nsend_a.at[span(theirs)], nrecv_a.at[mine], na_send.at[k], na_recv.at[mine], target)

    def y_out_b(k, mine, theirs, target):
        return copy(nsend_b.at[span(theirs)], nrecv_b.at[mine], nb_send.at[k], nb_recv.at[mine], target)

    full_a[:, :DV] = acc_a[...].T
    full_a[:, DV:] = acc_v[...].T
    nsend_a[...] = full_a[...].astype(BF)
    for k, peer in enumerate(y_peers):
        y_out_a(k, y, y_slots[k], peer).start()
    full_b[...] = acc_b[...].T
    nsend_b[...] = full_b[...].astype(BF)

    def home_a_wait(slot):
        copy(send_a.at[0], home_a.at[slot], ra_send.at[0], ha_recv.at[slot], below).wait_recv()
        own_a[...] += home_a[slot].astype(F32)

    def home_b_wait(slot):
        copy(send_b.at[0], home_b.at[slot], rb_send.at[0], hb_recv.at[slot], above).wait_recv()
        own_b[...] += home_b[slot].astype(F32)

    for slot in range(1, NZ):

        @pl.when(z + slot < NZ)
        def _(slot=slot):
            home_b_wait(slot)

    total_a = full_a[span(y), :]
    for k, peer in enumerate(y_peers):
        y_out_a(k, y_slots[k], y, peer).wait_recv()
        total_a += nrecv_a[y_slots[k]].astype(F32)
    gv = jnp.concatenate([total_a[:, DV:].astype(BF), own_b[:, DV:].astype(BF)], axis=1)
    gvg[y] = gv

    def gv_copy(k, mine, target):
        return copy(gvg.at[y], gvg.at[mine], gv_send.at[k], gv_recv.at[mine], target)

    for k, peer in enumerate(y_peers):
        gv_copy(k, y, peer).start()
    for k, peer in enumerate(y_peers):
        y_out_b(k, y, y_slots[k], peer).start()

    width = wv_ref.shape[0] // (2 * NX)

    def dl_part(tp_index):
        first = pl.multiple_of(tp_index * width, width)
        return lax.dot_general(
            gv, wv_ref[pl.ds(first, width), :], (((1,), (1,)), ((), ())), preferred_element_type=F32
        )

    def core_copy(j):
        return copy_to(dl_send.at[j], dl_core.at[j], dc_send.at[j], dc_recv.at[j], other_core)

    def x_copy(k, mine, theirs):
        return copy_to(dl_pair.at[theirs], dl_recv.at[mine], dx_send.at[k], dx_recv.at[mine], x_peers[k])

    for j in range(NX):
        dl_send[j] = dl_part(2 * j + 1 - core).astype(BF)
        core_copy(j).start()

    gk_ref[:, :DV] = total_a[:, :DV]
    gk_ref[:, DV:] = own_b[:, :DV]
    for k in range(NX):
        j = (x + k + 1) % NX
        mine = dl_part(2 * j + core)
        core_copy(j).wait_recv()
        dl_pair[j] = (mine + dl_core[j].astype(F32)).astype(BF)
        if k < NX - 1:
            x_copy(k, x, j).start()

    for k, peer in enumerate(y_peers):
        gv_copy(k, y_slots[k], peer).wait_recv()
        lat_copy(k, y_slots[k], y, peer).wait_recv()
    dw = dot(latg[0].T, gvg[0])
    for j in range(1, NY):
        dw += dot(latg[j].T, gvg[j])
    for j in range(NZ):
        dw_send[j] = dw[j * block : (j + 1) * block].astype(BF)

    def dw_copy(k, mine, theirs, target):
        return copy(dw_send.at[theirs], dw_recv.at[mine], dw_ssem.at[k], dw_rsem.at[mine], target)

    for k, peer in enumerate(z_peers):
        dw_copy(k, z, z_slots[k], peer).start()

    for slot in range(1, NZ):

        @pl.when(z - slot >= 0)
        def _(slot=slot):
            home_a_wait(slot)

    total_b = full_b[span(y), :]
    for k, peer in enumerate(y_peers):
        y_out_b(k, y_slots[k], y, peer).wait_recv()
        total_b += nrecv_b[y_slots[k]].astype(F32)
    gq_ref[:, :DV] = own_a[...]
    gq_ref[:, DV:] = total_b

    gl = dl_pair[x].astype(F32)
    for k in range(NX - 1):
        x_copy(k, x_slots[k], x).wait_recv()
        gl += dl_recv[x_slots[k]].astype(F32)
    gl_ref[...] = gl.astype(BF)

    gw = dw_send[z].astype(F32)
    for k, peer in enumerate(z_peers):
        dw_copy(k, z_slots[k], z, peer).wait_recv()
        gw += dw_recv[z_slots[k]].astype(F32)
    gw_ref[...] = gw

    for k, peer in enumerate(y_peers):
        for c in y_copies(k, y, peer):
            c().wait_send()
        lat_copy(k, y, y_slots[k], peer).wait_send()
        gv_copy(k, y, peer).wait_send()
        y_out_a(k, y, y, peer).wait_send()
        y_out_b(k, y, y, peer).wait_send()
    for k, peer in enumerate(z_peers):
        dw_copy(k, z, z_slots[k], peer).wait_send()
    for j in range(NX):
        core_copy(j).wait_send()
    for k in range(NX - 1):
        x_copy(k, x, x_slots[k]).wait_send()

    def sent(copies):
        for c in copies:
            c.wait_send()

    @pl.when(z > CHAIN)
    def _():
        sent(ma_copies(ma.at[z], sta.at[z], z, lowest, 1))

    @pl.when(z < NZ - 1 - CHAIN)
    def _():
        sent(mb_copies(mb.at[z], z, highest, 1))

    def drain_a(t, carry):
        @pl.when(t > 0)
        def _():
            home_a_copy(t).wait_send()

        @pl.when(jnp.logical_or(chains_a(t), t > CHAIN + 1))
        def _():
            sent(ma_copies(ma.at[z + t], sta.at[z + t], z + t, below))

        return carry

    def drain_b(t, carry):
        @pl.when(t > 0)
        def _():
            home_b_copy(t).wait_send()

        @pl.when(jnp.logical_or(chains_b(t), t > CHAIN + 1))
        def _():
            sent(mb_copies(mb.at[z - t], z - t, above))

        return carry

    lax.fori_loop(0, NZ - z, drain_a, 0)
    lax.fori_loop(0, z + 1, drain_b, 0)


def attention(queries, key_vectors, latents, value_weight, log_sums, out_first, out_second, cotangent, head_lambda):
    rows = queries.shape[0]
    wide = NY * rows
    depth = latents.shape[1]
    piece = depth // (NY * NZ)
    part = depth // (2 * NX)
    dma = pltpu.SemaphoreType.DMA
    vmem = pltpu.VMEM
    whole = pl.BlockSpec(memory_space=pltpu.VMEM)
    both = (rows, 2 * DV)
    stats = (8, rows + -rows % 128)
    return pl.pallas_call(
        attention_kernel,
        out_shape=(
            jax.ShapeDtypeStruct(both, F32),
            jax.ShapeDtypeStruct(both, F32),
            jax.ShapeDtypeStruct((rows, part), BF),
            jax.ShapeDtypeStruct((piece, 2 * DV), F32),
        ),
        in_specs=[whole] * 8 + [pl.BlockSpec(memory_space=pltpu.SMEM)],
        out_specs=(whole,) * 4,
        scratch_shapes=[
            vmem((NZ,) + both, BF),
            vmem((NZ,) + both, BF),
            vmem((NZ,) + stats, F32),
            vmem((NY,) + stats, F32),
            vmem((wide, DV), F32),
            vmem((stats[0], wide), F32),
            vmem((wide, 2 * DV), BF),
            vmem((wide, 2 * DV), BF),
            vmem((DV, wide), BF),
            vmem((DV, wide), BF),
            vmem((DV, wide), BF),
            vmem((DV, wide), BF),
            vmem((DV, wide), F32),
            vmem((DV, wide), F32),
            vmem((DV, wide), F32),
            vmem((rows, DV), F32),
            vmem(both, F32),
            vmem((wide, 2 * DV), F32),
            vmem((wide, DV), F32),
            vmem((NZ, rows, DV), BF),
            vmem((NZ,) + both, BF),
            vmem((NZ, rows, DV), BF),
            vmem((NZ,) + both, BF),
            vmem((wide, 2 * DV), BF),
            vmem((wide, DV), BF),
            vmem((NY,) + both, BF),
            vmem((NY, rows, DV), BF),
            vmem((rows, depth), BF),
            vmem((NY, rows, NZ * piece), BF),
            vmem((NY,) + both, BF),
            vmem((NZ, piece, 2 * DV), BF),
            vmem((NZ, piece, 2 * DV), BF),
            vmem((NX, rows, part), BF),
            vmem((NX, rows, part), BF),
            vmem((NX, rows, part), BF),
            vmem((NX, rows, part), BF),
            dma((NY - 1, 3)),
            dma((NY, 3)),
        ]
        + [dma((NZ, 2 * PIECES)), dma((NZ, PIECES)), dma((NZ, 2)), dma((NZ,))]
        + [dma((NZ, 2 * PIECES)), dma((NZ, PIECES))]
        + [dma((NZ,))] * 4
        + [dma((NY,))] * 8
        + [dma((NZ,))] * 2
        + [dma((NX,))] * 4,
        compiler_params=pltpu.CompilerParams(
            collective_id=0, has_side_effects=True, vmem_limit_bytes=60 * 1024 * 1024
        ),
        cost_estimate=pl.CostEstimate(flops=20_000_000_000, bytes_accessed=4_000_000, transcendentals=6_000_000),
    )(queries, key_vectors, latents, value_weight, log_sums, out_first, out_second, cotangent, head_lambda)


def per_device(
    queries,
    key_vectors,
    latents,
    value_weight,
    log_sums,
    out_first,
    out_second,
    cotangent,
    head_lambda,
):
    grad_queries, grad_keys, grad_latents, grad_weight = attention(
        queries, key_vectors, latents, value_weight, log_sums.T, out_first, out_second, cotangent, head_lambda
    )
    scale = DH ** (-0.5)
    grad_queries, grad_keys = grad_queries * scale, grad_keys * scale
    return (grad_queries, grad_keys, grad_latents, grad_weight)


def solution(mesh):
    return jax.shard_map(
        per_device,
        mesh=mesh,
        in_specs=(
            P("sp", "tp"),
            P("sp", "tp"),
            P("sp", None),
            P(None, "tp"),
            P("sp", "tp"),
            P("sp", "tp"),
            P("sp", "tp"),
            P("sp", "tp"),
            P("tp"),
        ),
        out_specs=(P("sp", "tp"), P("sp", "tp"), P("sp", "tp"), P("sp", "tp")),
        check_vma=False,
    )
```

```python
import functools
import math

import jax
import jax.numpy as jnp
from jax import lax
from jax.experimental import pallas as pl
from jax.experimental.pallas import tpu as pltpu
from jax.sharding import PartitionSpec as P

DH = 64
DV = 128
NY = 4
NZ = 8
NX = 4
PIECES = 1
HOME = (1, 3, 5, 6, 7)
CHAIN = 4
LOG2E = math.log2(math.e)
BF = jnp.bfloat16
F32 = jnp.float32


def dot(a, b):
    return jnp.dot(a, b, preferred_element_type=F32)


def low_map(x):
    return lax.broadcasted_iota(jnp.int32, x.shape, 1) < DH


def score_terms(m_a, m_b, na_t, nb_t, shift0, shift1, dot0, dot1, mask):
    low = low_map(m_a)
    none = jnp.zeros_like(m_a)
    s0 = dot(jnp.where(low, m_a, none), na_t) * (LOG2E * DH ** (-0.5)) - shift0
    s1 = dot(jnp.where(low, none, m_a), na_t) * (LOG2E * DH ** (-0.5)) - shift1
    da = dot(m_b, nb_t)
    if mask is not None:
        s0 = jnp.where(mask, s0, -1e30)
        s1 = jnp.where(mask, s1, -1e30)
    p0 = jnp.exp2(s0)
    p1 = jnp.exp2(s1)
    ds0 = (p0 * (da - dot0)).astype(BF)
    ds1 = (p1 * (dot1 - da)).astype(BF)
    weights = (p0 - p1).astype(BF)
    return ds0, ds1, weights


def attention_kernel(
    q_ref, k_ref, lat_ref, wv_ref, lse_ref, first_ref, second_ref, cot_ref, lam_ref,
    gq_ref, gk_ref, gl_ref, gw_ref,
    ma, mb, sta, stb, stc, stw, na, nb, nat, nvt, nbt, ndt,
    acc_a, acc_v, acc_b, own_a, own_b, full_a, full_b,
    send_a, send_b, home_a, home_b, pair_a, pair_b, nsend_a, nsend_b, nrecv_a, nrecv_b,
    lperm, latg, gvg, dw_send, dw_recv, dl_send, dl_core, dl_pair, dl_recv,
    yg_send, yg_recv, ma_send, ma_recv, sta_send, sta_recv, mb_send, mb_recv,
    ra_send, rb_send, ha_recv, hb_recv, rk_send, hk_recv, pa_recv, pb_recv,
    na_send, na_recv, nb_send, nb_recv,
    lat_send, lat_recv, gv_send, gv_recv, dw_ssem, dw_rsem, dc_send, dc_recv, dx_send, dx_recv,
):
    rows = q_ref.shape[0]
    wide = NY * rows
    sp = lax.axis_index("sp")
    tp = lax.axis_index("tp")
    z = sp // NY
    y = sp % NY
    x = tp // 2
    core = tp % 2

    def copy_to(src, dst, ssem, rsem, where):
        return pltpu.make_async_remote_copy(
            src_ref=src, dst_ref=dst, send_sem=ssem, recv_sem=rsem,
            device_id=where, device_id_type=pl.DeviceIdType.MESH,
        )

    def copy(src, dst, ssem, rsem, target):
        return copy_to(src, dst, ssem, rsem, {"sp": target})

    barrier = pltpu.get_barrier_semaphore()
    y_slots = [(y + k) % NY for k in range(1, NY)]
    z_slots = [(z + k) % NZ for k in range(1, NZ)]
    x_slots = [(x + k) % NX for k in range(1, NX)]
    y_peers = [z * NY + s for s in y_slots]
    z_peers = [s * NY + y for s in z_slots]
    other_core = {"tp": x * 2 + 1 - core}
    x_peers = [{"tp": s * 2 + core} for s in x_slots]
    everyone = [{"sp": p} for p in y_peers + z_peers] + [other_core] + x_peers
    for peer in everyone:
        pl.semaphore_signal(barrier, inc=1, device_id=peer, device_id_type=pl.DeviceIdType.MESH)

    def span(index):
        return pl.ds(pl.multiple_of(index * rows, rows), rows)

    last = NZ * NY - 1
    below = jnp.maximum(sp - NY, 0)
    above = jnp.minimum(sp + NY, last)
    lowest = y
    highest = (NZ - 1) * NY + y

    piece = rows // PIECES

    def ma_copies(src, st, c, target, far=0):
        return [copy(st, sta.at[c], sta_send.at[c, far], sta_recv.at[c], target)] + [
            copy(
                src.at[p * piece : (p + 1) * piece],
                ma.at[c, p * piece : (p + 1) * piece],
                ma_send.at[c, far * PIECES + p],
                ma_recv.at[c, p],
                target,
            )
            for p in range(PIECES)
        ]

    def mb_copies(src, c, target, far=0):
        return [
            copy(
                src.at[p * piece : (p + 1) * piece],
                mb.at[c, p * piece : (p + 1) * piece],
                mb_send.at[c, far * PIECES + p],
                mb_recv.at[c, p],
                target,
            )
            for p in range(PIECES)
        ]

    def y_copies(k, slot, target):
        return [
            lambda: copy(na.at[span(y)], na.at[span(slot)], yg_send.at[k, 0], yg_recv.at[slot, 0], target),
            lambda: copy(nb.at[span(y)], nb.at[span(slot)], yg_send.at[k, 1], yg_recv.at[slot, 1], target),
            lambda: copy(stb.at[y], stb.at[slot], yg_send.at[k, 2], yg_recv.at[slot, 2], target),
        ]

    def start(copies):
        for c in copies:
            c.start()

    values = dot(lat_ref[...], wv_ref[...]).astype(BF)
    k_own = k_ref[...]
    q_own = q_ref[...]
    which = lax.broadcasted_iota(jnp.int32, (rows, DV), 1)

    def row_terms(h):
        cols = slice(h * DV, (h + 1) * DV)
        first = first_ref[:, cols].astype(F32)
        second = second_ref[:, cols].astype(F32)
        grad_out = cot_ref[:, cols].astype(F32)
        lam = jnp.full((rows, 1), lam_ref[h], F32)
        mixed = first - lam * second
        inverse = lax.rsqrt(jnp.mean(mixed * mixed, axis=-1, keepdims=True) + 1e-06)
        normed = mixed * inverse
        mean = jnp.mean(grad_out * normed, axis=-1, keepdims=True)
        grad_rows = (inverse * (grad_out - normed * mean)).astype(BF)
        widened = grad_rows.astype(F32)
        dot0 = jnp.sum(widened * first, axis=-1, keepdims=True)
        dot1 = jnp.sum(widened * second, axis=-1, keepdims=True)
        stats = jnp.where(which < 3, dot0, dot1)
        stats = jnp.concatenate([stats, jnp.zeros((sta.shape[2] - rows, DV), F32)], axis=0)
        return grad_rows, stats.T[: sta.shape[1]]

    def shifts(h, m):
        shift = lse_ref[2 * h + m : 2 * h + m + 1, :] * LOG2E
        if m == 1:
            shift -= jnp.log(jnp.full((1, rows), lam_ref[h], F32)) * LOG2E
        return shift

    na[span(y), :DV] = k_own[:, :DV]
    na[span(y), DV:] = values[:, :DV]
    mb[z, :, :DV] = k_own[:, DV:]
    mb[z, :, DV:] = values[:, DV:]
    grad_rows, stats = row_terms(0)
    ma[z, :, :DV] = q_own[:, :DV]
    ma[z, :, DV:] = grad_rows
    sta[z] = stats
    sta[z, 0:1, :rows] = shifts(0, 0)
    sta[z, 1:2, :rows] = shifts(0, 1)
    grad_rows, stats = row_terms(1)
    nb[span(y), :DV] = q_own[:, DV:]
    nb[span(y), DV:] = grad_rows
    stb[y] = stats
    stb[y, 0:1, :rows] = shifts(1, 0)
    stb[y, 1:2, :rows] = shifts(1, 1)
    block = lat_ref.shape[1] // (NY * NZ)
    quarter = NZ * block
    for j in range(NY):
        for i in range(0, NZ, 2):
            one = (i * NY + j) * block
            two = (i * NY + NY + j) * block
            lperm[:, j * quarter + i * block : j * quarter + (i + 2) * block] = jnp.concatenate(
                [lat_ref[:, one : one + block], lat_ref[:, two : two + block]], axis=1
            )

    pl.semaphore_wait(barrier, len(everyone))

    @pl.when(z > 0)
    def _():
        start(ma_copies(ma.at[z], sta.at[z], z, below))

    @pl.when(z < NZ - 1)
    def _():
        start(mb_copies(mb.at[z], z, above))

    @pl.when(z > CHAIN)
    def _():
        start(ma_copies(ma.at[z], sta.at[z], z, lowest, 1))

    @pl.when(z < NZ - 1 - CHAIN)
    def _():
        start(mb_copies(mb.at[z], z, highest, 1))

    y_gather = [y_copies(k, y, peer) for k, peer in enumerate(y_peers)]
    for part in range(3):
        for k in range(NY - 1):
            y_gather[k][part]().start()

    def columns(index):
        return pl.ds(pl.multiple_of(index * quarter, quarter), quarter)

    def y_arrived(part):
        for k, peer in enumerate(y_peers):
            y_copies(k, y_slots[k], peer)[part]().wait_recv()

    def take_a(t):
        for c in ma_copies(ma.at[z + t], sta.at[z + t], z + t, below):
            c.wait_recv()

    def take_b(t):
        for c in mb_copies(mb.at[z - t], z - t, above):
            c.wait_recv()

    def pass_a(t):
        @pl.when(jnp.logical_and(jnp.logical_and(z > 0, t < CHAIN), z + t < NZ))
        def _():
            for c in ma_copies(ma.at[z + t], sta.at[z + t], z + t, below):
                c.wait_recv()
                c.start()

    def pass_b(t):
        @pl.when(jnp.logical_and(jnp.logical_and(z < NZ - 1, t < CHAIN), z - t >= 0))
        def _():
            for c in mb_copies(mb.at[z - t], z - t, above):
                c.wait_recv()
                c.start()

    def unit_a(m, stats, mask):
        st = stats.T[:rows]
        m_a = m[:, :DV]
        m_b = m[:, DV:]
        ds0, ds1, weights = score_terms(
            m_a, m_b, nat[...], nvt[...], st[:, 0:1], st[:, 1:2], st[:, 2:3], st[:, 3:4], mask
        )
        k_all = na[:, :DV]
        d0 = dot(ds0, k_all)
        d1 = dot(ds1, k_all)
        m_at = m_a.T
        parts = (dot(m_at[:DH], ds0), dot(m_at[DH:], ds1), dot(m_b.T, weights))
        return jnp.where(low_map(d0), d0, d1), parts

    def unit_b(m, mask):
        st = stw[...]
        m_a = m[:, :DV]
        m_b = m[:, DV:]
        ds0, ds1, weights = score_terms(
            m_a, m_b, nbt[...], ndt[...], st[0:1], st[1:2], st[2:3], st[3:4], mask
        )
        q_all = nb[:, :DV]
        d0 = dot(ds0, q_all)
        d1 = dot(ds1, q_all)
        dv = dot(weights, nb[:, DV:])
        m_at = m_a.T
        parts = (dot(m_at[:DH], ds0), dot(m_at[DH:], ds1))
        return jnp.where(low_map(d0), d0, d1), dv, parts

    lane = lax.broadcasted_iota(jnp.int32, (rows, wide), 1)
    place = lax.broadcasted_iota(jnp.int32, (rows, wide), 0) + y * rows

    def lat_copy(k, mine, theirs, target):
        return copy(lperm.at[:, columns(theirs)], latg.at[mine], lat_send.at[k], lat_recv.at[mine], target)

    latg[y] = lperm[:, columns(y)]
    acc_a[...] = jnp.zeros_like(acc_a)
    acc_v[...] = jnp.zeros_like(acc_v)
    acc_b[...] = jnp.zeros_like(acc_b)
    pass_a(1)
    pass_b(1)
    y_arrived(0)
    nat[...] = na[:, :DV].T
    nvt[...] = na[:, DV:].T

    def home_a_copy(t):
        return copy(
            send_a.at[t], home_a.at[t], ra_send.at[t], ha_recv.at[t], jnp.minimum(sp + t * NY, last)
        )

    def home_b_copies(t):
        target = jnp.maximum(sp - t * NY, 0)
        return [
            copy(send_b.at[t, :, DV:], home_b.at[t, :, DV:], rb_send.at[t], hb_recv.at[t], target),
            copy(send_b.at[t, :, :DV], home_b.at[t, :, :DV], rk_send.at[t], hk_recv.at[t], target),
        ]

    def pair_a_copy(t):
        return copy(send_a.at[t], pair_a.at[t], ra_send.at[t], pa_recv.at[t], above)

    def pair_b_copy(t):
        return copy(send_b.at[t], pair_b.at[t], rb_send.at[t], pb_recv.at[t], below)

    def chains_a(t):
        return jnp.logical_and(t < CHAIN, z > 0)

    def chains_b(t):
        return jnp.logical_and(t < CHAIN, z < NZ - 1)

    def step(n, carry):
        odd = n % 2
        t = (1 - odd) * (NZ - n // 2)
        t = jnp.where(n == 0, 0, t)
        t = jnp.where(n == 1, 2, t)
        t = jnp.where(n == 3, 1, t)
        t = jnp.where(n == 5, 4, t)
        t = jnp.where(n == 7, 3, t)
        meets = jnp.logical_or(t == 1, t == 3)
        joins = jnp.logical_or(t == 2, t == 4)
        home = jnp.logical_and(t > 0, jnp.logical_not(joins))
        all_seen = jnp.where(t == 0, 0, NY * rows)

        @pl.when(z + t < NZ)
        def _():
            @pl.when(jnp.logical_and(jnp.logical_not(chains_a(t)), t > 0))
            def _():
                take_a(t)

            @pl.when(t > CHAIN + 1)
            def _():
                start(ma_copies(ma.at[z + t], sta.at[z + t], z + t, above))

            moved, parts = unit_a(ma[z + t], sta[z + t], place + all_seen >= lane)
            acc_a[:DH] += parts[0]
            acc_a[DH:] += parts[1]
            acc_v[...] += parts[2]

            @pl.when(jnp.logical_and(meets, z > 0))
            def _():
                pair_a_copy(t + 1).wait_recv()
                send_a[t] = (moved + pair_a[t + 1].astype(F32)).astype(BF)

            @pl.when(jnp.logical_not(jnp.logical_and(meets, z > 0)))
            def _():
                send_a[t] = moved.astype(BF)

            @pl.when(joins)
            def _():
                pair_a_copy(t).start()

            @pl.when(home)
            def _():
                home_a_copy(t).start()

            @pl.when(t == 0)
            def _():
                own_a[...] = moved

        @pl.when(n < 2)
        def _():
            pass_a(n + 2)
            pass_b(n + 2)

        @pl.when(n == 0)
        def _():
            y_arrived(1)
            y_arrived(2)
            nbt[...] = nb[:, :DV].T
            ndt[...] = nb[:, DV:].T
            for j in range(NY):
                stc[j * rows : (j + 1) * rows, : stb.shape[1]] = stb[j].T[:rows]
            stw[...] = stc[...].T[: stw.shape[0]]
            for k, peer in enumerate(y_peers):
                lat_copy(k, y, y_slots[k], peer).start()

        @pl.when(z - t >= 0)
        def _():
            @pl.when(jnp.logical_and(jnp.logical_not(chains_b(t)), t > 0))
            def _():
                take_b(t)

            @pl.when(t > CHAIN + 1)
            def _():
                start(mb_copies(mb.at[z - t], z - t, below))

            moved, moved_v, parts = unit_b(mb[z - t], lane + all_seen >= place)
            acc_b[:DH] += parts[0]
            acc_b[DH:] += parts[1]

            @pl.when(jnp.logical_and(meets, z < NZ - 1))
            def _():
                pair_b_copy(t + 1).wait_recv()
                send_b[t, :, :DV] = (moved + pair_b[t + 1, :, :DV].astype(F32)).astype(BF)
                send_b[t, :, DV:] = (moved_v + pair_b[t + 1, :, DV:].astype(F32)).astype(BF)

            @pl.when(jnp.logical_not(jnp.logical_and(meets, z < NZ - 1)))
            def _():
                send_b[t, :, :DV] = moved.astype(BF)
                send_b[t, :, DV:] = moved_v.astype(BF)

            @pl.when(joins)
            def _():
                pair_b_copy(t).start()

            @pl.when(home)
            def _():
                home_b_copies(t)[0].start()

            @pl.when(t == 0)
            def _():
                own_b[:, :DV] = moved
                own_b[:, DV:] = moved_v

        return carry

    lax.fori_loop(0, NZ, step, 0)

    def y_out_a(k, mine, theirs, target):
        return copy(nsend_a.at[span(theirs)], nrecv_a.at[mine], na_send.at[k], na_recv.at[mine], target)

    def y_out_b(k, mine, theirs, target):
        return copy(nsend_b.at[span(theirs)], nrecv_b.at[mine], nb_send.at[k], nb_recv.at[mine], target)

    full_a[:, :DV] = acc_a[...].T
    full_a[:, DV:] = acc_v[...].T
    nsend_a[...] = full_a[...].astype(BF)
    for k, peer in enumerate(y_peers):
        y_out_a(k, y, y_slots[k], peer).start()
    full_b[...] = acc_b[...].T
    nsend_b[...] = full_b[...].astype(BF)
    for k, peer in enumerate(y_peers):
        y_out_b(k, y, y_slots[k], peer).start()
    for t in HOME:

        @pl.when(z - t >= 0)
        def _(t=t):
            home_b_copies(t)[1].start()

    def home_a_wait(slot):
        copy(send_a.at[0], home_a.at[slot], ra_send.at[0], ha_recv.at[slot], below).wait_recv()
        own_a[...] += home_a[slot].astype(F32)

    def home_b_wait(slot, part):
        sems = (hb_recv, hk_recv)[part]
        cols = (slice(DV, 2 * DV), slice(0, DV))[part]
        copy(
            send_b.at[0, :, cols], home_b.at[slot, :, cols], rb_send.at[0], sems.at[slot], above
        ).wait_recv()
        own_b[:, cols] += home_b[slot, :, cols].astype(F32)

    def gv_copy(k, mine, target, h):
        cols = slice(h * DV, (h + 1) * DV)
        return copy(
            gvg.at[y, :, cols], gvg.at[mine, :, cols], gv_send.at[k, h], gv_recv.at[mine, h], target
        )

    def dw_copy(k, mine, theirs, target, h):
        cols = slice(h * DV, (h + 1) * DV)
        return copy(
            dw_send.at[theirs, :, cols], dw_recv.at[mine, :, cols], dw_ssem.at[k, h], dw_rsem.at[mine, h], target
        )

    def weight_part(h):
        for k, peer in enumerate(y_peers):
            gv_copy(k, y_slots[k], peer, h).wait_recv()
        cols = slice(h * DV, (h + 1) * DV)
        dw = dot(latg[0].T, gvg[0, :, cols])
        for j in range(1, NY):
            dw += dot(latg[j].T, gvg[j, :, cols])
        for j in range(NZ):
            dw_send[j, :, cols] = dw[j * block : (j + 1) * block].astype(BF)
        for k, peer in enumerate(z_peers):
            dw_copy(k, z, z_slots[k], peer, h).start()

    total_a = full_a[span(y), :]
    for k, peer in enumerate(y_peers):
        y_out_a(k, y_slots[k], y, peer).wait_recv()
        total_a += nrecv_a[y_slots[k]].astype(F32)
    gvg[y, :, :DV] = total_a[:, DV:].astype(BF)
    for k, peer in enumerate(y_peers):
        gv_copy(k, y, peer, 0).start()
    for slot in HOME:

        @pl.when(z + slot < NZ)
        def _(slot=slot):
            home_b_wait(slot, 0)

    gvg[y, :, DV:] = own_b[:, DV:].astype(BF)
    for k, peer in enumerate(y_peers):
        gv_copy(k, y, peer, 1).start()
    gv = gvg[y]

    width = wv_ref.shape[0] // (2 * NX)

    def dl_part(tp_index):
        first = pl.multiple_of(tp_index * width, width)
        return lax.dot_general(
            gv, wv_ref[pl.ds(first, width), :], (((1,), (1,)), ((), ())), preferred_element_type=F32
        )

    def core_copy(j):
        return copy_to(dl_send.at[j], dl_core.at[j], dc_send.at[j], dc_recv.at[j], other_core)

    def x_copy(k, mine, theirs):
        return copy_to(dl_pair.at[theirs], dl_recv.at[mine], dx_send.at[k], dx_recv.at[mine], x_peers[k])

    for j in range(NX):
        dl_send[j] = dl_part(2 * j + 1 - core).astype(BF)
        core_copy(j).start()

    for k in range(NX):
        j = (x + k + 1) % NX
        mine = dl_part(2 * j + core)
        core_copy(j).wait_recv()
        dl_pair[j] = (mine + dl_core[j].astype(F32)).astype(BF)
        if k < NX - 1:
            x_copy(k, x, j).start()

    for k, peer in enumerate(y_peers):
        lat_copy(k, y_slots[k], y, peer).wait_recv()
    weight_part(0)
    weight_part(1)

    for slot in HOME:

        @pl.when(z - slot >= 0)
        def _(slot=slot):
            home_a_wait(slot)

        @pl.when(z + slot < NZ)
        def _(slot=slot):
            home_b_wait(slot, 1)

    gk_ref[:, :DV] = total_a[:, :DV]
    gk_ref[:, DV:] = own_b[:, :DV]
    total_b = full_b[span(y), :]
    for k, peer in enumerate(y_peers):
        y_out_b(k, y_slots[k], y, peer).wait_recv()
        total_b += nrecv_b[y_slots[k]].astype(F32)
    gq_ref[:, :DV] = own_a[...]
    gq_ref[:, DV:] = total_b

    gl = dl_pair[x].astype(F32)
    for k in range(NX - 1):
        x_copy(k, x_slots[k], x).wait_recv()
        gl += dl_recv[x_slots[k]].astype(F32)
    gl_ref[...] = gl.astype(BF)

    gw = dw_send[z].astype(F32)
    for k, peer in enumerate(z_peers):
        dw_copy(k, z_slots[k], z, peer, 0).wait_recv()
        dw_copy(k, z_slots[k], z, peer, 1).wait_recv()
        gw += dw_recv[z_slots[k]].astype(F32)
    gw_ref[...] = gw

    for k, peer in enumerate(y_peers):
        for c in y_copies(k, y, peer):
            c().wait_send()
        lat_copy(k, y, y_slots[k], peer).wait_send()
        gv_copy(k, y, peer, 0).wait_send()
        gv_copy(k, y, peer, 1).wait_send()
        y_out_a(k, y, y, peer).wait_send()
        y_out_b(k, y, y, peer).wait_send()
    for k, peer in enumerate(z_peers):
        dw_copy(k, z, z_slots[k], peer, 0).wait_send()
        dw_copy(k, z, z_slots[k], peer, 1).wait_send()
    for j in range(NX):
        core_copy(j).wait_send()
    for k in range(NX - 1):
        x_copy(k, x, x_slots[k]).wait_send()

    def sent(copies):
        for c in copies:
            c.wait_send()

    @pl.when(z > CHAIN)
    def _():
        sent(ma_copies(ma.at[z], sta.at[z], z, lowest, 1))

    @pl.when(z < NZ - 1 - CHAIN)
    def _():
        sent(mb_copies(mb.at[z], z, highest, 1))

    def drain_a(t, carry):
        @pl.when(t > 0)
        def _():
            home_a_copy(t).wait_send()

        @pl.when(jnp.logical_or(chains_a(t), t > CHAIN + 1))
        def _():
            sent(ma_copies(ma.at[z + t], sta.at[z + t], z + t, below))

        return carry

    def drain_b(t, carry):
        joins = jnp.logical_or(t == 2, t == 4)

        @pl.when(joins)
        def _():
            pair_b_copy(t).wait_send()

        @pl.when(jnp.logical_and(t > 0, jnp.logical_not(joins)))
        def _():
            sent(home_b_copies(t))

        @pl.when(jnp.logical_or(chains_b(t), t > CHAIN + 1))
        def _():
            sent(mb_copies(mb.at[z - t], z - t, above))

        return carry

    lax.fori_loop(0, NZ - z, drain_a, 0)
    lax.fori_loop(0, z + 1, drain_b, 0)


def attention(queries, key_vectors, latents, value_weight, log_sums, out_first, out_second, cotangent, head_lambda):
    rows = queries.shape[0]
    wide = NY * rows
    depth = latents.shape[1]
    piece = depth // (NY * NZ)
    part = depth // (2 * NX)
    dma = pltpu.SemaphoreType.DMA
    vmem = pltpu.VMEM
    whole = pl.BlockSpec(memory_space=pltpu.VMEM)
    both = (rows, 2 * DV)
    stats = (8, rows + -rows % 128)
    return pl.pallas_call(
        attention_kernel,
        out_shape=(
            jax.ShapeDtypeStruct(both, F32),
            jax.ShapeDtypeStruct(both, F32),
            jax.ShapeDtypeStruct((rows, part), BF),
            jax.ShapeDtypeStruct((piece, 2 * DV), F32),
        ),
        in_specs=[whole] * 8 + [pl.BlockSpec(memory_space=pltpu.SMEM)],
        out_specs=(whole,) * 4,
        scratch_shapes=[
            vmem((NZ,) + both, BF),
            vmem((NZ,) + both, BF),
            vmem((NZ,) + stats, F32),
            vmem((NY,) + stats, F32),
            vmem((wide, DV), F32),
            vmem((stats[0], wide), F32),
            vmem((wide, 2 * DV), BF),
            vmem((wide, 2 * DV), BF),
            vmem((DV, wide), BF),
            vmem((DV, wide), BF),
            vmem((DV, wide), BF),
            vmem((DV, wide), BF),
            vmem((DV, wide), F32),
            vmem((DV, wide), F32),
            vmem((DV, wide), F32),
            vmem((rows, DV), F32),
            vmem(both, F32),
            vmem((wide, 2 * DV), F32),
            vmem((wide, DV), F32),
            vmem((NZ, rows, DV), BF),
            vmem((NZ,) + both, BF),
            vmem((NZ, rows, DV), BF),
            vmem((NZ,) + both, BF),
            vmem((CHAIN + 1, rows, DV), BF),
            vmem((CHAIN + 1,) + both, BF),
            vmem((wide, 2 * DV), BF),
            vmem((wide, DV), BF),
            vmem((NY,) + both, BF),
            vmem((NY, rows, DV), BF),
            vmem((rows, depth), BF),
            vmem((NY, rows, NZ * piece), BF),
            vmem((NY,) + both, BF),
            vmem((NZ, piece, 2 * DV), BF),
            vmem((NZ, piece, 2 * DV), BF),
            vmem((NX, rows, part), BF),
            vmem((NX, rows, part), BF),
            vmem((NX, rows, part), BF),
            vmem((NX, rows, part), BF),
            dma((NY - 1, 3)),
            dma((NY, 3)),
        ]
        + [dma((NZ, 2 * PIECES)), dma((NZ, PIECES)), dma((NZ, 2)), dma((NZ,))]
        + [dma((NZ, 2 * PIECES)), dma((NZ, PIECES))]
        + [dma((NZ,))] * 6
        + [dma((CHAIN + 1,))] * 2
        + [dma((NY,))] * 6
        + [dma((NY, 2))] * 2
        + [dma((NZ, 2))] * 2
        + [dma((NX,))] * 4,
        compiler_params=pltpu.CompilerParams(
            collective_id=0, has_side_effects=True, vmem_limit_bytes=60 * 1024 * 1024
        ),
        cost_estimate=pl.CostEstimate(flops=20_000_000_000, bytes_accessed=4_000_000, transcendentals=6_000_000),
    )(queries, key_vectors, latents, value_weight, log_sums, out_first, out_second, cotangent, head_lambda)


def per_device(
    queries,
    key_vectors,
    latents,
    value_weight,
    log_sums,
    out_first,
    out_second,
    cotangent,
    head_lambda,
):
    grad_queries, grad_keys, grad_latents, grad_weight = attention(
        queries, key_vectors, latents, value_weight, log_sums.T, out_first, out_second, cotangent, head_lambda
    )
    scale = DH ** (-0.5)
    grad_queries, grad_keys = grad_queries * scale, grad_keys * scale
    return (grad_queries, grad_keys, grad_latents, grad_weight)


def solution(mesh):
    return jax.shard_map(
        per_device,
        mesh=mesh,
        in_specs=(
            P("sp", "tp"),
            P("sp", "tp"),
            P("sp", None),
            P(None, "tp"),
            P("sp", "tp"),
            P("sp", "tp"),
            P("sp", "tp"),
            P("sp", "tp"),
            P("tp"),
        ),
        out_specs=(P("sp", "tp"), P("sp", "tp"), P("sp", "tp"), P("sp", "tp")),
        check_vma=False,
    )
```
